32 devices in a mesh: ep: 32 (over z, y, x, core).
Axes of the slice: x: 2, y: 2, z: 4, core: 2. Of those that a mesh axis runs over, the one named last changes fastest.
Arguments:
- tokens: bfloat16 [512, 2048], P('ep'), may hold values from -6 to 6
- lengths: int32 [512], P('ep'), may hold values from 1 to 1024, 262144 in all
- cache_keys: bfloat16 [512, 1024, 128], P('ep'), may hold values from -6 to 6
- cache_values: bfloat16 [512, 1024, 128], P('ep'), may hold values from -6 to 6
- mix_gain: float32 [2048], replicated, may hold values from 0.1 to 1.9
- mix_out_gain: float32 [2048], replicated, may hold values from 0.1 to 1.9
- ffn_gain: float32 [2048], replicated, may hold values from 0.1 to 1.9
- ffn_out_gain: float32 [2048], replicated, may hold values from 0.1 to 1.9
- query_weight: bfloat16 [2048, 2048], P(None, 'ep'), may hold values from -0.125 to 0.125
- key_weight: bfloat16 [2048, 128], replicated, may hold values from -0.125 to 0.125
- value_weight: bfloat16 [2048, 128], replicated, may hold values from -0.125 to 0.125
- head_bias: float32 [32], replicated, may hold values from -8 to -2
- output_weight: bfloat16 [2048, 2048], P(None, 'ep'), may hold values from -0.125 to 0.125
- routes: int32 [512, 6], P('ep'), may hold values from 0 to 31, all different within a row; in each aligned block of 16 rows (0 to 15, 16 to 31, ...) at most 6 rows name the same one
- route_weights: float32 [512, 6], P('ep'), may hold values from 0.1 to 1
- expert_gate: bfloat16 [32, 2048, 512], P('ep'), may hold values from -0.125 to 0.125
- expert_up: bfloat16 [32, 2048, 512], P('ep'), may hold values from -0.125 to 0.125
- expert_down: bfloat16 [32, 512, 2048], P('ep'), may hold values from -0.25 to 0.25
- shared_gate: bfloat16 [2048, 512], replicated, may hold values from -0.125 to 0.125
- shared_up: bfloat16 [2048, 512], replicated, may hold values from -0.125 to 0.125
- shared_down: bfloat16 [512, 2048], replicated, may hold values from -0.25 to 0.25
Outputs:
- layer_out: bfloat16 [512, 2048], P('ep')
- new_keys: bfloat16 [512, 128], P('ep')
- new_values: bfloat16 [512, 128], P('ep')
The draws below stay inside these ranges and needn't reach their ends.
Inputs may be any that keep to these rules, and one draw needn't show every extreme that they name: `routes`: each row names 6 different experts. Among the rows of one device no expert is named more than 6 times, a bound that some block reaches in some device's rows. `lengths`: the new token stands at this position; cache entries at this position and after are unused. Some sequence has exactly 1024.
All inputs are finite; a program needn't handle non-finite values. No bound on the sum of `lengths` on one device may be relied on, other than what follows from the above.
Results may differ from the reference program's by a relative error of at most 0.013.
Values may be sent and summed in bfloat16 or wider, within the bound.
A program may use at most 128 MiB of HBM per device.

```python
import math
import jax
import jax.numpy as jnp
import numpy as np
from jax import lax

D = 2048
HD = 64
H = 32
KV = 2
FF = 512
SFF = 512
TOP_K = 6
SEQ_DEV = 16
LEN = 1024
TOKENS = 512
EXPERTS = 32
CAP = 6
N_EP = 32


def shard_levels(rng, shape, split, smallest, largest):
    def one(dim, shards_of):
        draws = jax.random.uniform(jax.random.fold_in(jax.random.fold_in(rng, 6), dim), (shards_of,), jnp.float32, smallest / len(split), largest / len(split))
        return jnp.repeat(jnp.exp(draws), shape[dim] // shards_of).reshape((-1,) + (1,) * (len(shape) - dim - 1))

    level = one(*split[0])
    for cut in split[1:]:
        level = level * one(*cut)
    return level


def length_profile(number_of, total, bound, skew):
    weights = [(1 << 20) // math.isqrt(standing ** skew) + 1 for standing in range(2, number_of + 1)]
    spare, given = total - bound - (number_of - 1), [1] * (number_of - 1)
    while spare > 0:
        candidates = [i for i in range(number_of - 1) if given[i] < bound]
        mass, remaining = sum([weights[i] for i in candidates]), spare
        for i in candidates:
            more = min(bound - given[i], max(1, remaining * weights[i] // mass), spare)
            given[i] = given[i] + more
            spare = spare - more
    return np.array([bound] + given)


def ragged_sizes(key, amount, total, limit, slope):
    if amount == 2:
        one = jax.random.randint(key, (), max(1, total - limit), min(limit, total - 1) + 1)
        return jnp.stack([one, total - one])
    tallies = jnp.asarray(length_profile(amount, total, limit, slope), jnp.int32)
    pairs = (amount - 1) // 2
    source_of, taker = tallies[1:1 + 2 * pairs:2], tallies[2:2 + 2 * pairs:2]
    slack = jnp.minimum(source_of - 1, limit - taker)
    moved = jax.random.randint(jax.random.fold_in(key, 1), (pairs,), 0, 1 << 20) % (slack + 1)
    tallies = tallies.at[1:1 + 2 * pairs:2].set(source_of - moved).at[2:2 + 2 * pairs:2].set(taker + moved)
    return tallies[jax.random.permutation(jax.random.fold_in(key, 2), amount)]


def routed_block(rng, own, number, rows, amount, top, reach, lean):
    order = jax.random.permutation(rng, amount)
    heavy_load, ordinary = portions_of(amount, rows * top, reach, lean, True), portions_of(amount, rows * top, reach, lean, False)
    places = jnp.arange(amount)

    def named(tallies, offset_by):
        used = int((tallies > 0).sum())
        fixed = max(1, used // 4)
        shifted = fixed + (places - fixed + offset_by * (used - fixed)) % max(1, amount - fixed)
        return jnp.zeros((amount,), jnp.int32).at[order[jnp.where(places < fixed, places, shifted)]].set(jnp.asarray(tallies, jnp.int32))

    tallies = jnp.where(number % 4 == 0, named(heavy_load, number // 4), named(ordinary, number - number // 4 - 1))
    mixed = jax.random.permutation(jax.random.fold_in(own, 3), amount)
    giver, taker = mixed[0:amount // 2 * 2:2], mixed[1:amount // 2 * 2:2]
    room = jnp.minimum(tallies[giver] - 1, reach - tallies[taker]) // 2
    room = jnp.where((giver == order[0]) | (taker == order[0]) | (tallies[taker] == 0), 0, jnp.maximum(room, 0))
    shifted = jax.random.randint(jax.random.fold_in(own, 4), (amount // 2,), 0, 1 << 20) % (room + 1)
    tallies = tallies.at[giver].add(-shifted).at[taker].add(shifted)
    members = jnp.searchsorted(jnp.cumsum(tallies), jnp.arange(rows * top), side="right").astype(jnp.int32)
    grid = members.reshape(top, rows).T
    grid = grid[jax.random.permutation(jax.random.fold_in(own, 1), rows)]
    offset_by = jax.random.randint(jax.random.fold_in(own, 2), (rows, 1), 0, top)
    return jnp.take_along_axis(grid, (jnp.arange(top)[None, :] + offset_by) % top, axis=1)


def portions_of(amount, total, reach, slope, full):
    portions = [(1 << 20) // math.isqrt(standing ** slope) + 1 for standing in range(1, amount + 1)]
    largest = reach if full else min(reach, max(-(-total // amount), total * portions[0] // sum(portions)))
    least = 1 if total - largest >= amount - 1 else 0
    holding, spare = [largest] + [least] * (amount - 1), total - largest - least * (amount - 1)
    while spare > 0:
        candidates = [i for i in range(1, amount) if holding[i] < largest] or [i for i in range(1, amount) if holding[i] < reach]
        whole, remaining = sum([portions[i] for i in candidates]), spare
        for i in candidates:
            more = min(reach - holding[i], max(1, remaining * portions[i] // whole), spare)
            holding[i] = holding[i] + more
            spare = spare - more
    return np.array(holding)


def noise(rng, dims, scale, bound, shards=(), held_as=jnp.bfloat16):
    values = scale * jax.random.normal(rng, dims, jnp.float32)
    if shards:
        values = values * shard_levels(rng, dims, shards, -0.22, 0.18)
    return jnp.clip(values, -bound, bound).astype(held_as)


def setup_inputs(seed: int = 0) -> dict:
    arg_keys = jax.random.split(jax.random.key(seed), 22)
    tokens = noise(arg_keys[0], (TOKENS, D), 1.0, 6.0, ((0, 32),))
    lengths = ragged_sizes(arg_keys[1], TOKENS, TOKENS * LEN // 2, LEN, 2).astype(jnp.int32)
    cache_keys = noise(arg_keys[2], (TOKENS, LEN, KV * HD), 1.0, 6.0, ((0, 32),))
    cache_values = noise(arg_keys[3], (TOKENS, LEN, KV * HD), 1.0, 6.0, ((0, 32),))
    mix_gain = jnp.clip(1.0 + 0.18 * jax.random.normal(arg_keys[4], (D,), jnp.float32), 0.1, 1.9)
    mix_out_gain = jnp.clip(1.0 + 0.18 * jax.random.normal(arg_keys[5], (D,), jnp.float32), 0.1, 1.9)
    ffn_gain = jnp.clip(1.0 + 0.18 * jax.random.normal(arg_keys[6], (D,), jnp.float32), 0.1, 1.9)
    ffn_out_gain = jnp.clip(1.0 + 0.18 * jax.random.normal(arg_keys[7], (D,), jnp.float32), 0.1, 1.9)
    query_weight = noise(arg_keys[8], (D, D), D ** -0.5, 0.125, ((1, 32),))
    key_weight = noise(arg_keys[9], (D, KV * HD), D ** -0.5, 0.125)
    value_weight = noise(arg_keys[10], (D, KV * HD), D ** -0.5, 0.125)
    head_bias = jnp.clip(jax.random.uniform(arg_keys[11], (H,), jnp.float32, -8.0, -2.0), -8.0, -2.0)
    output_weight = noise(arg_keys[12], (D, D), D ** -0.5, 0.125, ((1, 32),))
    routes_keys = jax.random.split(jax.random.fold_in(arg_keys[13], 1), TOKENS // SEQ_DEV)
    routes_turns = jax.random.permutation(jax.random.fold_in(arg_keys[13], 3), TOKENS // SEQ_DEV)
    routes = jax.vmap(lambda own, number: routed_block(jax.random.fold_in(arg_keys[13], 2), own, number, SEQ_DEV, EXPERTS, TOP_K, CAP, 2))(routes_keys, routes_turns).reshape((TOKENS, TOP_K))
    route_weights = jnp.clip(jnp.exp(math.log(1.0) - 2.3025851 * jax.random.uniform(arg_keys[14], (TOKENS, TOP_K), jnp.float32) ** shard_levels(arg_keys[14], (TOKENS, TOP_K), ((0, 32),), -0.2, 0.2)), 0.1, 1.0)
    expert_gate = noise(arg_keys[15], (EXPERTS, D, FF), D ** -0.5, 0.125, ((0, 32),))
    expert_up = noise(arg_keys[16], (EXPERTS, D, FF), D ** -0.5, 0.125, ((0, 32),))
    expert_down = noise(arg_keys[17], (EXPERTS, FF, D), FF ** -0.5, 0.25, ((0, 32),))
    shared_gate = noise(arg_keys[18], (D, SFF), D ** -0.5, 0.125)
    shared_up = noise(arg_keys[19], (D, SFF), D ** -0.5, 0.125)
    shared_down = noise(arg_keys[20], (SFF, D), SFF ** -0.5, 0.25)
    return dict(tokens=tokens, lengths=lengths, cache_keys=cache_keys, cache_values=cache_values, mix_gain=mix_gain, mix_out_gain=mix_out_gain, ffn_gain=ffn_gain, ffn_out_gain=ffn_out_gain, query_weight=query_weight, key_weight=key_weight, value_weight=value_weight, head_bias=head_bias, output_weight=output_weight, routes=routes, route_weights=route_weights, expert_gate=expert_gate, expert_up=expert_up, expert_down=expert_down, shared_gate=shared_gate, shared_up=shared_up, shared_down=shared_down)


def rms_scale(rows, gain):
    return rows * lax.rsqrt(lax.optimization_barrier(jnp.mean(rows * rows, axis=-1, keepdims=True)) + 1e-06) * gain

def attend_block(items, head_bias):
    queries, keys, values, lens = items
    seqs = queries.shape[0]
    group = H // KV
    q4 = queries.reshape(seqs, KV, group, HD).astype(jnp.float32)
    k4 = keys.reshape(seqs, LEN, KV, HD).astype(jnp.float32)
    v4 = values.reshape(seqs, LEN, KV, HD).astype(jnp.float32)
    scores = jnp.einsum('skgd,slkd->skgl', q4, k4) * HD ** (-0.5)
    scores = scores + head_bias.reshape(KV, group)[None, :, :, None]
    valid = (jnp.arange(LEN)[None, :] < lens[:, None])[:, None, None, :]
    log_beta = jax.nn.log_sigmoid(scores)
    log_keep = jnp.where(valid, log_beta - scores, 0.0)
    after = lax.cumsum(log_keep, axis=3, reverse=True) - log_keep
    weights = jnp.where(valid, jnp.exp(log_beta + after), 0.0).astype(jnp.bfloat16)
    out = jnp.einsum('skgl,slkd->skgd', weights.astype(jnp.float32), v4)
    return out.astype(jnp.bfloat16).reshape(seqs, H * HD)

def reference(tokens, lengths, cache_keys, cache_values, mix_gain, mix_out_gain, ffn_gain, ffn_out_gain, query_weight, key_weight, value_weight, head_bias, output_weight, routes, route_weights, expert_gate, expert_up, expert_down, shared_gate, shared_up, shared_down):
    resid = tokens.astype(jnp.float32)
    normed = rms_scale(resid, mix_gain).astype(jnp.bfloat16)
    new_keys = jnp.dot(normed, key_weight, preferred_element_type=jnp.float32).astype(jnp.bfloat16)
    new_values = jnp.dot(normed, value_weight, preferred_element_type=jnp.float32).astype(jnp.bfloat16)
    queries = jnp.dot(normed, query_weight, preferred_element_type=jnp.float32).astype(jnp.bfloat16)
    blocks = TOKENS // SEQ_DEV
    attended = lax.map(lambda items: attend_block(items, head_bias), (queries.reshape(blocks, SEQ_DEV, D), cache_keys.reshape(blocks, SEQ_DEV, LEN, KV * HD), cache_values.reshape(blocks, SEQ_DEV, LEN, KV * HD), lengths.reshape(blocks, SEQ_DEV)))
    attended = attended.reshape(TOKENS, D)
    mixed = jnp.dot(attended, output_weight, preferred_element_type=jnp.float32).astype(jnp.bfloat16)
    resid1 = resid + rms_scale(mixed.astype(jnp.float32), mix_out_gain)
    ffn_in = rms_scale(resid1, ffn_gain).astype(jnp.bfloat16)
    shared_hidden = (jax.nn.silu(jnp.dot(ffn_in, shared_gate, preferred_element_type=jnp.float32)) * jnp.dot(ffn_in, shared_up, preferred_element_type=jnp.float32)).astype(jnp.bfloat16)
    shared_out = jnp.dot(shared_hidden, shared_down, preferred_element_type=jnp.float32)
    flat = routes.reshape(-1)
    onehot = (flat[:, None] == jnp.arange(EXPERTS)[None, :]).astype(jnp.int32)
    onehot = onehot.reshape(N_EP, SEQ_DEV * TOP_K, EXPERTS)
    rank = lax.optimization_barrier(jnp.sum((jnp.cumsum(onehot, axis=1) - onehot) * onehot, axis=2)).reshape(-1)
    assign = jnp.arange(TOKENS * TOP_K)
    source = assign // (SEQ_DEV * TOP_K)
    row_index = (source * CAP + rank).astype(jnp.int32)
    token_of = (assign // TOP_K).astype(jnp.int32)
    table = jnp.full((EXPERTS, N_EP * CAP), TOKENS, jnp.int32).at[flat, row_index].set(token_of)
    weight_table = jnp.zeros((EXPERTS, N_EP * CAP), jnp.float32).at[flat, row_index].set(route_weights.reshape(-1))
    padded = jnp.concatenate([ffn_in, jnp.zeros((1, D), jnp.bfloat16)], axis=0)

    def one_expert(carry, items):
        ids, wts, w_gate, w_up, w_down = items
        rows = padded[ids]
        hidden = (jax.nn.silu(jnp.dot(rows, w_gate, preferred_element_type=jnp.float32)) * jnp.dot(rows, w_up, preferred_element_type=jnp.float32)).astype(jnp.bfloat16)
        result = jnp.dot(hidden, w_down, preferred_element_type=jnp.float32).astype(jnp.bfloat16)
        return (carry.at[ids].add(result.astype(jnp.float32) * wts[:, None]), None)
    routed, unused = lax.scan(one_expert, jnp.zeros((TOKENS + 1, D), jnp.float32), (table, weight_table, expert_gate, expert_up, expert_down))
    routed = routed[:TOKENS]
    layer_out = (resid1 + rms_scale(routed + shared_out, ffn_out_gain)).astype(jnp.bfloat16)
    return (layer_out, new_keys, new_values)
```

```python
import functools

import jax
import jax.numpy as jnp
from jax import lax
from jax.experimental import pallas as pl
from jax.experimental.pallas import tpu as pltpu
from jax.sharding import PartitionSpec as P

HD = 64
LANES = 128
F32 = jnp.float32
BF16 = jnp.bfloat16


def rms_scale(rows, gain):
    return rows * lax.rsqrt(jnp.mean(rows * rows, axis=-1, keepdims=True) + 1e-06) * gain


def dot(a, b):
    return jnp.dot(a, b, preferred_element_type=F32)


def loop(start, stop, one):
    def step(i, carry):
        one(i)
        return carry

    lax.fori_loop(start, stop, step, 0)


def remote(src, dst, send_sem, recv_sem, device):
    return pltpu.make_async_remote_copy(
        src_ref=src,
        dst_ref=dst,
        send_sem=send_sem,
        recv_sem=recv_sem,
        device_id=(device,),
        device_id_type=pl.DeviceIdType.MESH,
    )


class Place:
    def __init__(self, n):
        me = lax.axis_index("ep")
        self.n, self.lines = n, n // 4
        self.chip, self.core = me // 2, me % 2
        self.partner = 2 * self.chip + (1 - self.core)
        self.z, self.q = self.chip // 4, self.chip % 4
        self.qx = self.q + 1 - 2 * (self.q % 2)
        self.qy = self.q + 2 - 4 * (self.q // 2)
        self.qd = 3 - self.q

    def device(self, chip):
        return 2 * chip + self.core

    def back_z(self, i):
        return (self.z + self.lines - i) % self.lines


class Direct:
    def __init__(self, here, buf, send_sems, recv_sems):
        self.here, self.buf, self.send_sems, self.recv_sems = here, buf, send_sems, recv_sems

    def send(self, src, chip):
        here = self.here
        remote(
            src, self.buf.at[here.chip], self.send_sems.at[chip],
            self.recv_sems.at[here.chip], here.device(chip),
        ).start()

    def wait(self, chip):
        remote(
            self.buf.at[chip], self.buf.at[chip], self.send_sems.at[chip],
            self.recv_sems.at[chip], self.here.partner,
        ).wait_recv()

    def wait_sent(self, chip):
        remote(
            self.buf.at[chip], self.buf.at[chip], self.send_sems.at[chip],
            self.recv_sems.at[chip], self.here.partner,
        ).wait_send()

    def others(self, one):
        here = self.here
        loop(1, here.n, lambda i: one((here.chip + i) % here.n))


class Gather:
    def __init__(self, here, buf, send_sems, recv_sems):
        self.here, self.buf, self.send_sems, self.recv_sems = here, buf, send_sems, recv_sems

    def copy(self, src, slot, kind, index, chip):
        return remote(
            src, self.buf.at[slot], self.send_sems.at[kind, index],
            self.recv_sems.at[slot], self.here.device(chip),
        )

    def to_quad(self, src, slot, kind, q):
        self.copy(src, slot, kind, slot, 4 * self.here.z + q).start()

    def start(self, src):
        here = self.here
        self.to_quad(src, here.chip, 1, here.qx)
        self.to_quad(src, here.chip, 2, here.qy)

        def line(i):
            to = 4 * ((here.z + i) % here.lines) + here.q
            self.copy(src, here.chip, 0, i, to).start()

        loop(1, here.lines, line)

    def wait(self, slot):
        here = self.here
        self.copy(self.buf.at[slot], slot, 0, 0, 4 * here.z + here.qx).wait_recv()

    def column(self, i, process):
        here = self.here
        slot = 4 * here.back_z(i) + here.q
        self.wait(slot)
        self.to_quad(self.buf.at[slot], slot, 1, here.qx)
        self.to_quad(self.buf.at[slot], slot, 2, here.qy)
        process(slot)

    def sides(self, i, process):
        here = self.here
        z = here.back_z(i)
        for q, parity, kind, to in ((here.qx, 0, 2, here.qy), (here.qy, 1, 1, here.qx)):
            slot = 4 * z + q
            self.wait(slot)

            @pl.when(z % 2 == parity)
            def _():
                self.to_quad(self.buf.at[slot], slot, kind, to)

            process(slot)

    def forward(self, process):
        here = self.here

        def both(i):
            self.column(i, process)
            self.sides(i - 1, process)

        loop(1, here.lines, both)
        self.sides(here.lines - 1, process)

    def diagonal(self, i):
        slot = 4 * self.here.back_z(i) + self.here.qd
        self.wait(slot)
        return slot

    def finish(self):
        here = self.here

        def sent(kind, index):
            self.copy(self.buf.at[0], 0, kind, index, 4 * here.z + here.qx).wait_send()

        loop(1, here.lines, lambda i: sent(0, i))

        def rest(z):
            for kind in (1, 2):
                sent(kind, 4 * z + here.q)

            @pl.when(z % 2 == 0)
            def _():
                sent(2, 4 * z + here.qx)

            @pl.when(z % 2 == 1)
            def _():
                sent(1, 4 * z + here.qy)

        loop(0, here.lines, rest)


def project(here, rows, own_rows, weight, outs, out_send):
    outs.buf[here.chip] = dot(own_rows[...], weight[...]).astype(BF16)

    def process(slot):
        out_send[slot] = dot(rows.buf[slot], weight[...]).astype(BF16)
        outs.send(out_send.at[slot], slot)

    rows.forward(process)
    loop(0, here.lines, lambda i: process(rows.diagonal(i)))
    outs.others(outs.wait)
    return jnp.concatenate([outs.buf[i] for i in range(here.n)], axis=1)


def attend(lens, bias, tri, queries, keys, values, q_seq, o_seq):
    seqs, span, width = keys.shape
    pairs = q_seq.shape[1]
    for j in range(pairs):
        q_seq[:, j, :] = queries[:, j * LANES:(j + 1) * LANES].astype(F32)
    low = lax.broadcasted_iota(jnp.int32, (pairs, LANES), 1) < HD
    front = lax.broadcasted_iota(jnp.int32, (pairs, LANES), 0) < pairs // 2
    used = low == front
    heads = 2 * pairs
    count = span // LANES
    pos = lax.broadcasted_iota(jnp.int32, (heads, span), 1)

    def one(s):
        a = q_seq[s]
        r = pltpu.roll(a, HD, 1)
        even = jnp.where(used, jnp.where(front, a, r), 0.0)
        odd = jnp.where(used, jnp.where(front, r, a), 0.0)
        q = jnp.concatenate([even, odd], axis=0).astype(BF16)
        z = lax.dot_general(q, keys[s], (((1,), (1,)), ((), ())), preferred_element_type=F32)
        z = z * HD ** (-0.5) + bias[...]
        valid = pos < lens[s]
        soft = jnp.log(1.0 + jnp.exp(-jnp.abs(z)))
        log_beta = jnp.minimum(z, 0.0) - soft
        log_keep = jnp.where(valid, -jnp.maximum(z, 0.0) - soft, 0.0)
        high = log_keep.astype(BF16)
        rest = (log_keep - high.astype(F32)).astype(BF16)
        parts = [p[:, b * LANES:(b + 1) * LANES] for p in (high, rest) for b in range(count)]
        sums = dot(jnp.concatenate(parts, axis=0), tri[...])
        carry = jnp.zeros((heads, LANES), F32)
        after = [None] * count
        for b in reversed(range(count)):
            here = sums[b * heads:(b + 1) * heads] + sums[(count + b) * heads:(count + b + 1) * heads]
            after[b] = here[:, :LANES] + carry
            carry = carry + here[:, LANES:]
        stick = jnp.where(valid, jnp.exp(log_beta + jnp.concatenate(after, axis=1)), 0.0)
        out = dot(stick.astype(BF16), values[s])
        even, odd = out[:pairs], out[pairs:]
        even_r, odd_r = pltpu.roll(even, HD, 1), pltpu.roll(odd, HD, 1)
        o_seq[s] = jnp.where(
            low, jnp.where(front, even, even_r), jnp.where(front, odd_r, odd)
        )

    many = 4 if seqs % 4 == 0 else 1

    def some(i):
        for j in range(many):
            one(many * i + j)

    loop(0, seqs // many, some)
    return jnp.concatenate([o_seq[:, j, :] for j in range(pairs)], axis=1).astype(BF16)


def layer_kernel(
    n,
    lens, tok, g0, g1, g2, g3, bias_row, routes, route_weights, wq, wk, wv, wo, ck, cv, eg, eu, ed, sg, su, sd,
    joined,
    normed, rows_a, att, rows_b, ffn_in, rows_c, pair_q, weight_q, line_o,
    kw, vw, keys, values, tri, q_seq, o_seq,
    q_buf, q_out, o_buf, o_out, resid1, wts, wts_all, bias,
    gate, up, down, sgate, sup, sdown, total, ysend, quad_buf, line_send, line_buf,
    as_, ar, bs, br, cs, cr, qs, qr, os_, or_, ts, tr, ws, wr, us, ur, vs, vr, xs, xr, fs, fr, ls,
):
    here = Place(n)
    chip, core, partner = here.chip, here.core, here.partner
    seqs = tok.shape[0]
    ff = eg.shape[2]
    own = wq.shape[0]
    barrier = pltpu.get_barrier_semaphore()

    def hello(i):
        pl.semaphore_signal(barrier, inc=1, device_id=(here.device((chip + i) % n),))

    loop(1, n, hello)
    pl.semaphore_signal(barrier, inc=1, device_id=(partner,))
    mine = pl.ds(core * ff, ff)
    cols = pl.ds(core * own, own)
    local = [
        pltpu.make_async_copy(src, dst, ls.at[i])
        for i, (src, dst) in enumerate([
            (wq, pair_q.at[cols]), (wk, kw), (wv, vw), (ck, keys), (cv, values),
            (wo, line_o.at[here.z, cols]),
            (eg.at[0], gate.at[core]), (eu.at[0], up.at[core]), (ed.at[0], down.at[mine]),
            (sg, sgate), (su, sup), (sd, sdown),
        ])
    ]
    for copy in local:
        copy.start()
    normed[...] = rms_scale(tok[...].astype(F32), g0[...]).astype(BF16)
    after = lax.broadcasted_iota(jnp.int32, (LANES, 2 * LANES), 0) > lax.broadcasted_iota(
        jnp.int32, (LANES, 2 * LANES), 1
    )
    every = lax.broadcasted_iota(jnp.int32, (LANES, 2 * LANES), 1) >= LANES
    tri[...] = jnp.where(after | every, 1.0, 0.0).astype(BF16)
    heads = bias.shape[0]
    row = lax.broadcasted_iota(jnp.int32, (heads, heads), 0)
    head = jnp.where(row < heads // 2, 2 * row, 2 * row - heads + 1)
    at_head = lax.broadcasted_iota(jnp.int32, (heads, heads), 1) == head
    bias[...] = jnp.sum(jnp.where(at_head, bias_row[...], 0.0), axis=1, keepdims=True)
    expert = lax.broadcasted_iota(jnp.int32, (2 * n, seqs), 0)
    dense = jnp.zeros((2 * n, seqs), F32)
    for k in range(routes.shape[0]):
        dense = dense + jnp.where(
            routes[k:k + 1, :] == expert, route_weights[k:k + 1, :], 0.0
        )
    wts[...] = jnp.zeros_like(wts)
    for c in range(n):
        wts[c, :, :seqs] = dense[2 * c:2 * c + 2]
    pl.semaphore_wait(barrier, n)

    first = Gather(here, rows_a, as_, ar)
    third = Gather(here, rows_c, cs, cr)
    q_outs = Direct(here, q_buf, qs, qr)
    tabs = Direct(here, wts_all, ts, tr)
    swaps = [
        remote(src, dst, ws.at[i], wr.at[i], partner)
        for i, (src, dst) in enumerate([
            (wq, pair_q.at[cols]),
            (eg.at[0], gate.at[core]), (eu.at[0], up.at[core]), (ed.at[0], down.at[mine]),
        ])
    ]
    peers = (here.qx, here.qy, here.qd)

    def line_weight(src, slot, i, to):
        return remote(src, line_o.at[slot, cols], xs.at[i], xr.at[slot], here.device(4 * to + here.q))

    def pair_weight(src, slot):
        return remote(src, line_o.at[slot, cols], fs.at[slot], fr.at[slot], partner)

    def quad_rows(p):
        return remote(
            att, rows_b.at[here.q], bs.at[p], br.at[here.q], here.device(4 * here.z + peers[p])
        )

    def quad_outs(p):
        return remote(
            o_out.at[peers[p]], o_buf.at[here.q], os_.at[p], or_.at[here.q],
            here.device(4 * here.z + peers[p]),
        )

    first.start(normed)
    swaps[0].start()
    loop(1, here.lines, lambda i: line_weight(wo, here.z, i, (here.z + i) % here.lines).start())
    pair_weight(wo, here.z).start()
    for copy in swaps[1:]:
        copy.start()
    tabs.others(lambda c: tabs.send(wts.at[c], c))
    wts_all[chip] = wts[chip]
    for copy in local[:3]:
        copy.wait()
    wide, width = tok.shape[1], wk.shape[1]
    joined[:, wide:wide + width] = dot(normed[...], kw[...]).astype(BF16)
    joined[:, wide + width:] = dot(normed[...], vw[...]).astype(BF16)
    swaps[0].wait_recv()
    weight_q[...] = pair_q[...].T
    queries = project(here, first, normed, weight_q, q_outs, q_out)
    for copy in local[3:]:
        copy.wait()
    att[...] = attend(lens, bias, tri, queries, keys, values, q_seq, o_seq)

    for p in (2, 0, 1):
        quad_rows(p).start()

    def forward_weight(i):
        slot = here.back_z(i)
        line_weight(wo, slot, 0, here.z).wait_recv()
        pair_weight(line_o.at[slot, cols], slot).start()

    loop(1, here.lines, forward_weight)
    rows_b[here.q] = att[...]
    loop(0, here.lines, lambda z: pair_weight(wo, z).wait_recv())
    for p in range(3):
        remote(
            att, rows_b.at[peers[p]], bs.at[p], br.at[peers[p]], partner
        ).wait_recv()
    part = lax.dot_general(
        rows_b[...].reshape(4 * seqs, -1), line_o[...].reshape(2 * own * here.lines, -1),
        (((1,), (1,)), ((), ())), preferred_element_type=F32,
    ).astype(BF16)
    for q in range(4):
        o_out[q] = part[q * seqs:(q + 1) * seqs]
    for p in (2, 0, 1):
        quad_outs(p).start()
    o_buf[here.q] = o_out[here.q]
    for p in range(3):
        remote(
            o_out.at[0], o_buf.at[peers[p]], os_.at[p], or_.at[peers[p]], partner
        ).wait_recv()
    mixed = jnp.concatenate([
        o_buf[q, :, 2 * own * z:2 * own * (z + 1)] for z in range(here.lines) for q in range(4)
    ], axis=1)
    resid1[...] = tok[...].astype(F32) + rms_scale(mixed.astype(F32), g1[...])
    ffn_in[...] = rms_scale(resid1[...], g2[...]).astype(BF16)

    third.start(ffn_in)
    rows_c[chip] = ffn_in[...]
    mid = (jax.nn.silu(dot(ffn_in[...], sgate[...])) * dot(ffn_in[...], sup[...])).astype(BF16)
    total[...] = dot(mid, sdown[...])
    tabs.others(tabs.wait)
    for copy in swaps[1:]:
        copy.wait_recv()
    eye = (
        lax.broadcasted_iota(jnp.int32, (seqs, wts.shape[2]), 0)
        == lax.broadcasted_iota(jnp.int32, (seqs, wts.shape[2]), 1)
    )

    def quad_copy(p, z):
        return remote(
            ysend.at[4 * z + peers[p]], quad_buf.at[p, z], us.at[p, z], ur.at[p, z],
            here.device(4 * here.z + peers[p]),
        )

    def line_copy(i, slot, z):
        return remote(
            line_send.at[i], line_buf.at[slot], vs.at[i], vr.at[slot],
            here.device(4 * z + here.q),
        )

    def group(i):
        slots = [4 * here.back_z(i) + q for q in range(4)]
        x = jnp.concatenate([rows_c[slot] for slot in slots], axis=0)
        halves = []
        for e in range(2):
            columns = []
            for slot in slots:
                row = wts_all[slot][e:e + 1]
                columns.append(jnp.sum(jnp.where(eye, row, 0.0), axis=1, keepdims=True))
            scale = jnp.concatenate(columns, axis=0)
            hidden = jax.nn.silu(dot(x, gate[e])) * dot(x, up[e])
            halves.append((hidden * scale).astype(BF16))
        y = dot(jnp.concatenate(halves, axis=1), down[...]).astype(BF16)
        for j, slot in enumerate(slots):
            ysend[slot] = y[j * seqs:(j + 1) * seqs]
        for p in (2, 0, 1):
            quad_copy(p, here.back_z(i)).start()

    def quad_sum(i):
        z = here.back_z(i)
        acc = ysend[4 * z + here.q].astype(F32)
        for p in range(3):
            quad_copy(p, z).wait_recv()
            acc = acc + quad_buf[p, z].astype(F32)
        return z, acc

    def pass_on(i):
        z, acc = quad_sum(i)
        line_send[i] = acc.astype(BF16)
        line_copy(i, here.z, z).start()

    def stage(i):
        third.sides(i, lambda slot: None)

        @pl.when(i + 1 < here.lines)
        def _():
            third.column(i + 1, lambda slot: None)

        third.diagonal(i)
        group(i)

        @pl.when(i > 1)
        def _():
            pass_on(i - 1)

    loop(0, here.lines, stage)
    loop(max(here.lines - 1, 1), here.lines, pass_on)
    _, acc = quad_sum(0)
    total[...] += acc

    def add(i):
        z = (here.z + i) % here.lines
        line_copy(0, z, here.z).wait_recv()
        total[...] += line_buf[z].astype(F32)

    loop(1, here.lines, add)
    joined[:, :wide] = (resid1[...] + rms_scale(total[...], g3[...])).astype(BF16)

    for copy in swaps:
        copy.wait_send()
    for plane in (first, third):
        plane.finish()
    for plane in (q_outs, tabs):
        plane.others(plane.wait_sent)

    def sent(z):
        for p in range(3):
            quad_copy(p, z).wait_send()

    loop(0, here.lines, sent)
    loop(1, here.lines, lambda i: line_weight(wo, here.z, i, here.z).wait_send())
    loop(0, here.lines, lambda z: pair_weight(wo, z).wait_send())
    for p in range(3):
        quad_rows(p).wait_send()
        quad_outs(p).wait_send()
    loop(1, here.lines, lambda i: line_copy(i, 0, here.z).wait_send())


def split_kernel(joined, layer_out, new_keys, new_values):
    wide, keys = layer_out.shape[1], new_keys.shape[1]
    layer_out[...] = joined[:, :wide]
    new_keys[...] = joined[:, wide:wide + keys]
    new_values[...] = joined[:, wide + keys:]


def run_layer(n, lens, tokens, gains, bias, routes, route_weights, wq, wk, wv, wo, ck, cv, eg, eu, ed, sg, su, sd):
    vm = pl.BlockSpec(memory_space=pltpu.VMEM)
    hbm = pl.BlockSpec(memory_space=pl.ANY)
    seqs, wide = tokens.shape
    own = wq.shape[0]
    ff = eg.shape[2]
    lines = n // 4
    pairs = n * 2 * own // LANES
    sems = pltpu.SemaphoreType.DMA
    half = lambda *shape: pltpu.VMEM(shape, BF16)
    full = lambda *shape: pltpu.VMEM(shape, F32)
    joined = pl.pallas_call(
        functools.partial(layer_kernel, n),
        out_shape=jax.ShapeDtypeStruct((seqs, wide + wk.shape[1] + wv.shape[1]), BF16),
        in_specs=[pl.BlockSpec(memory_space=pltpu.SMEM)] + [vm] * 8 + [hbm] * 12,
        out_specs=vm,
        scratch_shapes=[
            half(seqs, wide), half(n, seqs, wide), half(seqs, wide), half(4, seqs, wide),
            half(seqs, wide), half(n, seqs, wide),
            half(2 * own, wide), half(wide, 2 * own), half(lines, 2 * own, wide),
            half(*wk.shape), half(*wv.shape), half(*ck.shape), half(*cv.shape),
            half(LANES, 2 * LANES), full(seqs, pairs, LANES), full(seqs, pairs, LANES),
            half(n, seqs, 2 * own), half(n, seqs, 2 * own),
            half(4, seqs, 2 * own * lines), half(4, seqs, 2 * own * lines),
            full(seqs, wide), full(n, 2, LANES), full(n, 2, LANES), full(bias.shape[1], 1),
            half(2, wide, ff), half(2, wide, ff), half(2 * ff, wide),
            half(*sg.shape), half(*su.shape), half(*sd.shape),
            full(seqs, wide), half(n, seqs, wide), half(3, lines, seqs, wide),
            half(lines, seqs, wide), half(lines, seqs, wide),
            sems((3, n)), sems((n,)), sems((3,)), sems((4,)), sems((3, n)), sems((n,)),
            sems((n,)), sems((n,)), sems((3,)), sems((4,)), sems((n,)), sems((n,)),
            sems((4,)), sems((4,)), sems((3, lines)), sems((3, lines)),
            sems((lines,)), sems((lines,)), sems((lines,)), sems((lines,)),
            sems((lines,)), sems((lines,)), sems((12,)),
        ],
        compiler_params=pltpu.CompilerParams(
            collective_id=0, has_side_effects=True, vmem_limit_bytes=62 << 20
        ),
    )(lens, tokens, *gains, bias, routes, route_weights, wq, wk, wv, wo, ck, cv, eg, eu, ed, sg, su, sd)
    return pl.pallas_call(
        split_kernel,
        out_shape=(
            jax.ShapeDtypeStruct((seqs, wide), BF16),
            jax.ShapeDtypeStruct((seqs, wk.shape[1]), BF16),
            jax.ShapeDtypeStruct((seqs, wv.shape[1]), BF16),
        ),
        in_specs=[vm],
        out_specs=(vm,) * 3,
    )(joined)


def body(
    tokens,
    lengths,
    cache_keys,
    cache_values,
    mix_gain,
    mix_out_gain,
    ffn_gain,
    ffn_out_gain,
    query_weight,
    key_weight,
    value_weight,
    head_bias,
    output_weight,
    routes,
    route_weights,
    expert_gate,
    expert_up,
    expert_down,
    shared_gate,
    shared_up,
    shared_down,
):
    n = lax.axis_size("ep") // 2
    gains = [g[None] for g in (mix_gain, mix_out_gain, ffn_gain, ffn_out_gain)]
    return run_layer(
        n, lengths, tokens, gains, head_bias[None], routes.T, route_weights.T, query_weight.T, key_weight, value_weight,
        output_weight.T, cache_keys, cache_values,
        expert_gate, expert_up, expert_down, shared_gate, shared_up, shared_down,
    )


def solution(mesh):
    in_specs = (
        P("ep", None),
        P("ep"),
        P("ep", None, None),
        P("ep", None, None),
        P(),
        P(),
        P(),
        P(),
        P(None, "ep"),
        P(),
        P(),
        P(),
        P(None, "ep"),
        P("ep", None),
        P("ep", None),
        P("ep", None, None),
        P("ep", None, None),
        P("ep", None, None),
        P(),
        P(),
        P(),
    )
    out_specs = (P("ep", None), P("ep", None), P("ep", None))
    return jax.shard_map(body, mesh=mesh, in_specs=in_specs, out_specs=out_specs, check_vma=False)
```

```python
import functools

import jax
import jax.numpy as jnp
from jax import lax
from jax.experimental import pallas as pl
from jax.experimental.pallas import tpu as pltpu
from jax.sharding import PartitionSpec as P

HD = 64
LANES = 128
F32 = jnp.float32
BF16 = jnp.bfloat16
Z_PER_GROUP = 2


def rms_scale(rows, gain):
    return rows * lax.rsqrt(jnp.mean(rows * rows, axis=-1, keepdims=True) + 1e-06) * gain


def dot(a, b):
    return jnp.dot(a, b, preferred_element_type=F32)


def loop(start, stop, one):
    def step(i, carry):
        one(i)
        return carry

    lax.fori_loop(start, stop, step, 0)


def remote(src, dst, send_sem, recv_sem, device):
    return pltpu.make_async_remote_copy(
        src_ref=src,
        dst_ref=dst,
        send_sem=send_sem,
        recv_sem=recv_sem,
        device_id=(device,),
        device_id_type=pl.DeviceIdType.MESH,
    )


class Place:
    def __init__(self, n):
        me = lax.axis_index("ep")
        self.n, self.lines = n, n // 4
        self.chip, self.core = me // 2, me % 2
        self.partner = 2 * self.chip + (1 - self.core)
        self.z, self.q = self.chip // 4, self.chip % 4
        self.qx = self.q + 1 - 2 * (self.q % 2)
        self.qy = self.q + 2 - 4 * (self.q // 2)
        self.qd = 3 - self.q

    def device(self, chip):
        return 2 * chip + self.core

    def back_z(self, i):
        return (self.z + self.lines - i) % self.lines


class Direct:
    def __init__(self, here, buf, send_sems, recv_sems):
        self.here, self.buf, self.send_sems, self.recv_sems = here, buf, send_sems, recv_sems

    def send(self, src, chip):
        here = self.here
        remote(
            src, self.buf.at[here.chip], self.send_sems.at[chip],
            self.recv_sems.at[here.chip], here.device(chip),
        ).start()

    def wait(self, chip):
        remote(
            self.buf.at[chip], self.buf.at[chip], self.send_sems.at[chip],
            self.recv_sems.at[chip], self.here.partner,
        ).wait_recv()

    def wait_sent(self, chip):
        remote(
            self.buf.at[chip], self.buf.at[chip], self.send_sems.at[chip],
            self.recv_sems.at[chip], self.here.partner,
        ).wait_send()

    def gathered(self):
        self.others(self.wait)
        return jnp.concatenate([self.buf[i] for i in range(self.here.n)], axis=1)

    def others(self, one):
        here = self.here
        loop(1, here.n, lambda i: one((here.chip + i) % here.n))


class Gather:
    def __init__(self, here, buf, send_sems, recv_sems):
        self.here, self.buf, self.send_sems, self.recv_sems = here, buf, send_sems, recv_sems

    def copy(self, src, slot, kind, index, chip):
        return remote(
            src, self.buf.at[slot], self.send_sems.at[kind, index],
            self.recv_sems.at[slot], self.here.device(chip),
        )

    def to_quad(self, src, slot, kind, q):
        self.copy(src, slot, kind, slot, 4 * self.here.z + q).start()

    def start(self, src):
        here = self.here
        self.to_quad(src, here.chip, 1, here.qx)
        self.to_quad(src, here.chip, 2, here.qy)

        def line(i):
            to = 4 * ((here.z + i) % here.lines) + here.q
            self.copy(src, here.chip, 0, i, to).start()

        loop(1, here.lines, line)

    def wait(self, slot):
        here = self.here
        self.copy(self.buf.at[slot], slot, 0, 0, 4 * here.z + here.qx).wait_recv()

    def column(self, i, process):
        here = self.here
        slot = 4 * here.back_z(i) + here.q
        self.wait(slot)
        self.to_quad(self.buf.at[slot], slot, 1, here.qx)
        self.to_quad(self.buf.at[slot], slot, 2, here.qy)
        process(slot)

    def sides(self, i, process):
        here = self.here
        z = here.back_z(i)
        for q, parity, kind, to in ((here.qx, 0, 2, here.qy), (here.qy, 1, 1, here.qx)):
            slot = 4 * z + q
            self.wait(slot)

            @pl.when(z % 2 == parity)
            def _():
                self.to_quad(self.buf.at[slot], slot, kind, to)

            process(slot)

    def forward(self, process):
        here = self.here

        def both(i):
            self.column(i, process)
            self.sides(i - 1, process)

        loop(1, here.lines, both)
        self.sides(here.lines - 1, process)

    def diagonal(self, i):
        slot = 4 * self.here.back_z(i) + self.here.qd
        self.wait(slot)
        return slot

    def finish(self):
        here = self.here

        def sent(kind, index):
            self.copy(self.buf.at[0], 0, kind, index, 4 * here.z + here.qx).wait_send()

        loop(1, here.lines, lambda i: sent(0, i))

        def rest(z):
            for kind in (1, 2):
                sent(kind, 4 * z + here.q)

            @pl.when(z % 2 == 0)
            def _():
                sent(2, 4 * z + here.qx)

            @pl.when(z % 2 == 1)
            def _():
                sent(1, 4 * z + here.qy)

        loop(0, here.lines, rest)


def project(here, rows, own_rows, weight, outs, out_send):
    outs.buf[here.chip] = dot(own_rows[...], weight[...]).astype(BF16)

    def process(slot):
        out_send[slot] = dot(rows.buf[slot], weight[...]).astype(BF16)
        outs.send(out_send.at[slot], slot)

    with jax.named_scope("qfwd"):
        rows.forward(process)
    with jax.named_scope("qdiag"):
        loop(0, here.lines, lambda i: process(rows.diagonal(i)))


def attend(lens, bias, tri, queries, keys, values, q_seq, o_seq, att, send_half, pass_weights):
    seqs, span, width = keys.shape
    pairs = q_seq.shape[1]
    for j in range(pairs):
        q_seq[:, j, :] = queries[:, j * LANES:(j + 1) * LANES].astype(F32)
    low = lax.broadcasted_iota(jnp.int32, (pairs, LANES), 1) < HD
    front = lax.broadcasted_iota(jnp.int32, (pairs, LANES), 0) < pairs // 2
    used = low == front
    heads = 2 * pairs
    count = span // LANES
    pos = lax.broadcasted_iota(jnp.int32, (heads, span), 1)

    def one(s):
        a = q_seq[s]
        r = pltpu.roll(a, HD, 1)
        even = jnp.where(used, jnp.where(front, a, r), 0.0)
        odd = jnp.where(used, jnp.where(front, r, a), 0.0)
        q = jnp.concatenate([even, odd], axis=0).astype(BF16)
        z = lax.dot_general(q, keys[s], (((1,), (1,)), ((), ())), preferred_element_type=F32)
        z = z * HD ** (-0.5) + bias[...]
        valid = pos < lens[s]
        soft = jnp.log(1.0 + jnp.exp(-jnp.abs(z)))
        log_beta = jnp.minimum(z, 0.0) - soft
        log_keep = jnp.where(valid, -jnp.maximum(z, 0.0) - soft, 0.0)
        high = log_keep.astype(BF16)
        rest = (log_keep - high.astype(F32)).astype(BF16)
        parts = [p[:, b * LANES:(b + 1) * LANES] for p in (high, rest) for b in range(count)]
        sums = dot(jnp.concatenate(parts, axis=0), tri[...])
        carry = jnp.zeros((heads, LANES), F32)
        after = [None] * count
        for b in reversed(range(count)):
            here = sums[b * heads:(b + 1) * heads] + sums[(count + b) * heads:(count + b + 1) * heads]
            after[b] = here[:, :LANES] + carry
            carry = carry + here[:, LANES:]
        stick = jnp.where(valid, jnp.exp(log_beta + jnp.concatenate(after, axis=1)), 0.0)
        out = dot(stick.astype(BF16), values[s])
        even, odd = out[:pairs], out[pairs:]
        even_r, odd_r = pltpu.roll(even, HD, 1), pltpu.roll(odd, HD, 1)
        o_seq[s] = jnp.where(
            low, jnp.where(front, even, even_r), jnp.where(front, odd_r, odd)
        )

    many = 4 if seqs % 4 == 0 else 1

    def some(i):
        for j in range(many):
            one(many * i + j)

    steps = seqs // many
    mid, late = steps // 2, max(steps // 2, steps - 1)

    def finish(h):
        rows = pl.ds(h * (seqs // 2), seqs // 2)
        att[rows] = jnp.concatenate([o_seq[rows, j, :] for j in range(pairs)], axis=1).astype(BF16)
        send_half(h)

    def stage(i):
        @pl.when(i == late)
        def _():
            pass_weights()

        some(i)

        @pl.when(i == mid - 1)
        def _():
            finish(0)

    loop(0, steps, stage)
    finish(1)


def layer_kernel(
    n,
    lens, tok, g0, g1, g2, g3, bias_row, routes, route_weights, wq, wk, wv, wo, ck, cv, eg, eu, ed, sg, su, sd,
    joined,
    normed, rows_a, att, rows_b, ffn_in, rows_c, pair_q, weight_q, quad_o,
    kw, vw, keys, values, tri, q_seq, o_seq,
    q_buf, q_out, o_buf, o_out, resid1, wts, wts_all, bias,
    gate, up, down, sgate, sup, sdown, total, ysend, quad_buf, line_send, line_buf,
    as_, ar, bs, br, cs, cr, qs, qr, os_, or_, ts, tr, ws, wr, us, ur, vs, vr, xs, xr, ys, yr, fs, fr, ls,
):
    here = Place(n)
    chip, core, partner = here.chip, here.core, here.partner
    seqs = tok.shape[0]
    ff = eg.shape[2]
    own = wq.shape[0]
    barrier = pltpu.get_barrier_semaphore()

    def hello(i):
        pl.semaphore_signal(barrier, inc=1, device_id=(here.device((chip + i) % n),))

    loop(1, n, hello)
    pl.semaphore_signal(barrier, inc=1, device_id=(partner,))
    mine = pl.ds(core * ff, ff)
    cols = pl.ds(core * own, own)
    local = [
        pltpu.make_async_copy(src, dst, ls.at[i])
        for i, (src, dst) in enumerate([
            (wq, pair_q.at[cols]), (wk, kw), (wv, vw), (ck, keys), (cv, values),
            (wo, quad_o.at[here.q, cols]),
            (eg.at[0], gate.at[core]), (eu.at[0], up.at[core]), (ed.at[0], down.at[mine]),
            (sg, sgate), (su, sup), (sd, sdown),
        ])
    ]
    for copy in local:
        copy.start()
    normed[...] = rms_scale(tok[...].astype(F32), g0[...]).astype(BF16)
    after = lax.broadcasted_iota(jnp.int32, (LANES, 2 * LANES), 0) > lax.broadcasted_iota(
        jnp.int32, (LANES, 2 * LANES), 1
    )
    every = lax.broadcasted_iota(jnp.int32, (LANES, 2 * LANES), 1) >= LANES
    tri[...] = jnp.where(after | every, 1.0, 0.0).astype(BF16)
    heads = bias.shape[0]
    row = lax.broadcasted_iota(jnp.int32, (heads, heads), 0)
    head = jnp.where(row < heads // 2, 2 * row, 2 * row - heads + 1)
    at_head = lax.broadcasted_iota(jnp.int32, (heads, heads), 1) == head
    bias[...] = jnp.sum(jnp.where(at_head, bias_row[...], 0.0), axis=1, keepdims=True)
    expert = lax.broadcasted_iota(jnp.int32, (2 * n, seqs), 0)
    dense = jnp.zeros((2 * n, seqs), F32)
    for k in range(routes.shape[0]):
        dense = dense + jnp.where(
            routes[k:k + 1, :] == expert, route_weights[k:k + 1, :], 0.0
        )
    wts[...] = jnp.zeros_like(wts)
    for c in range(n):
        wts[c, :, :seqs] = dense[2 * c:2 * c + 2]
    with jax.named_scope("barrier"):
        pl.semaphore_wait(barrier, n)

    first = Gather(here, rows_a, as_, ar)
    third = Gather(here, rows_c, cs, cr)
    q_outs = Direct(here, q_buf, qs, qr)
    tabs = Direct(here, wts_all, ts, tr)
    swaps = [
        remote(src, dst, ws.at[i], wr.at[i], partner)
        for i, (src, dst) in enumerate([
            (wq, pair_q.at[cols]),
            (eg.at[0], gate.at[core]), (eu.at[0], up.at[core]), (ed.at[0], down.at[mine]),
        ])
    ]
    peers = (here.qx, here.qy, here.qd)
    cut = own // 2
    part_of = seqs // 2

    def quad_weight(p):
        mine_o = quad_o.at[here.q, cols]
        return remote(mine_o, mine_o, xs.at[p], xr.at[p], here.device(4 * here.z + peers[p]))

    def quad_weight_in(p):
        there = quad_o.at[peers[p], cols]
        return remote(there, there, xs.at[p], xr.at[p], partner)

    def relay_weight(p):
        half_o = quad_o.at[peers[p], pl.ds(core * own + p * cut, cut)]
        return remote(half_o, half_o, ys.at[p], yr.at[p], here.device(4 * here.z + peers[1 - p]))

    def relay_weight_in(p):
        half_o = quad_o.at[here.qd, pl.ds(core * own + p * cut, cut)]
        return remote(half_o, half_o, ys.at[p], yr.at[p], partner)

    def pair_weight(q):
        held = quad_o.at[q, cols]
        return remote(held, held, fs.at[q], fr.at[q], partner)

    def pair_weight_in(q):
        held = quad_o.at[q, pl.ds((1 - core) * own, own)]
        return remote(held, held, fs.at[q], fr.at[q], partner)

    def line_rows(i, h):
        z = (here.z + i) % here.lines
        some = pl.ds(h * part_of, part_of)
        return remote(
            att.at[some], rows_b.at[here.z, some], bs.at[h, i], br.at[h, here.z],
            here.device(4 * z + here.q),
        )

    def line_rows_in(i, h):
        z = here.back_z(i)
        some = pl.ds(h * part_of, part_of)
        return remote(att.at[some], rows_b.at[z, some], bs.at[h, i], br.at[h, z], partner)

    def line_outs(i):
        z = (here.z + i) % here.lines
        return remote(
            o_out.at[z], o_buf.at[here.z], os_.at[i], or_.at[here.z], here.device(4 * z + here.q)
        )

    def line_outs_in(i):
        z = here.back_z(i)
        return remote(o_out.at[z], o_buf.at[z], os_.at[i], or_.at[z], partner)

    first.start(normed)
    for copy in swaps:
        copy.start()
    tabs.others(lambda c: tabs.send(wts.at[c], c))
    wts_all[chip] = wts[chip]
    for copy in local[:3]:
        copy.wait()
    wide, width = tok.shape[1], wk.shape[1]
    joined[:, wide:wide + width] = dot(normed[...], kw[...]).astype(BF16)
    joined[:, wide + width:] = dot(normed[...], vw[...]).astype(BF16)
    swaps[0].wait_recv()
    weight_q[...] = pair_q[...].T
    project(here, first, normed, weight_q, q_outs, q_out)
    for copy in local[3:]:
        copy.wait()
    quad_weight(0).start()
    quad_weight(1).start()
    pair_weight(here.q).start()
    with jax.named_scope("qret"):
        queries = q_outs.gathered()

    def send_half(h):
        some = pl.ds(h * part_of, part_of)
        rows_b[here.z, some] = att[some]
        loop(1, here.lines, lambda i: line_rows(i, h).start())

    def pass_weights():
        for p in range(2):
            quad_weight_in(p).wait_recv()
            relay_weight(p).start()
        for p in range(2):
            pair_weight(peers[p]).start()

    with jax.named_scope("attend"):
        attend(lens, bias, tri, queries, keys, values, q_seq, o_seq, att, send_half, pass_weights)

    with jax.named_scope("weights"):
        for p in range(2):
            relay_weight_in(p).wait_recv()
        pair_weight(here.qd).start()
        for q in range(4):
            pair_weight_in(q).wait_recv()

    with jax.named_scope("rows_b"):
        for h in range(2):
            loop(1, here.lines, lambda i: line_rows_in(i, h).wait_recv())
    with jax.named_scope("odot"):
        part = lax.dot_general(
            rows_b[...].reshape(here.lines * seqs, -1), quad_o[...].reshape(8 * own, -1),
            (((1,), (1,)), ((), ())), preferred_element_type=F32,
        ).astype(BF16)
        o_out[...] = part.reshape(here.lines, seqs, 8 * own)
    loop(1, here.lines, lambda i: line_outs(i).start())
    o_buf[here.z] = o_out[here.z]
    with jax.named_scope("oret"):
        loop(1, here.lines, lambda i: line_outs_in(i).wait_recv())
    mixed = jnp.concatenate([o_buf[z] for z in range(here.lines)], axis=1)
    resid1[...] = tok[...].astype(F32) + rms_scale(mixed.astype(F32), g1[...])
    ffn_in[...] = rms_scale(resid1[...], g2[...]).astype(BF16)

    third.start(ffn_in)
    rows_c[chip] = ffn_in[...]
    mid = (jax.nn.silu(dot(ffn_in[...], sgate[...])) * dot(ffn_in[...], sup[...])).astype(BF16)
    total[...] = dot(mid, sdown[...])
    tabs.others(tabs.wait)
    for copy in swaps[1:]:
        copy.wait_recv()
    with jax.named_scope("fwd3"):
        third.forward(lambda slot: None)
    per = Z_PER_GROUP if here.lines % Z_PER_GROUP == 0 else 1
    eye = (
        lax.broadcasted_iota(jnp.int32, (seqs, wts.shape[2]), 0)
        == lax.broadcasted_iota(jnp.int32, (seqs, wts.shape[2]), 1)
    )

    def quad_copy(p, z):
        return remote(
            ysend.at[4 * z + peers[p]], quad_buf.at[p, z], us.at[p, z], ur.at[p, z],
            here.device(4 * here.z + peers[p]),
        )

    def line_copy(i, slot, z):
        return remote(
            line_send.at[i], line_buf.at[slot], vs.at[i], vr.at[slot],
            here.device(4 * z + here.q),
        )

    def group(g):
        slots = []
        for j in range(per):
            i = g * per + j
            third.diagonal(i)
            slots += [4 * here.back_z(i) + q for q in range(4)]
        x = jnp.concatenate([rows_c[slot] for slot in slots], axis=0)
        halves = []
        for e in range(2):
            columns = []
            for slot in slots:
                row = wts_all[slot][e:e + 1]
                columns.append(jnp.sum(jnp.where(eye, row, 0.0), axis=1, keepdims=True))
            scale = jnp.concatenate(columns, axis=0)
            hidden = jax.nn.silu(dot(x, gate[e])) * dot(x, up[e])
            halves.append((hidden * scale).astype(BF16))
        y = dot(jnp.concatenate(halves, axis=1), down[...]).astype(BF16)
        for j, slot in enumerate(slots):
            ysend[slot] = y[j * seqs:(j + 1) * seqs]
        for j in reversed(range(per)):
            for p in (2, 0, 1):
                quad_copy(p, here.back_z(g * per + j)).start()

    def quad_sum(i):
        z = here.back_z(i)
        acc = ysend[4 * z + here.q].astype(F32)
        for p in range(3):
            quad_copy(p, z).wait_recv()
            acc = acc + quad_buf[p, z].astype(F32)
        return z, acc

    def pass_on(i):
        z, acc = quad_sum(i)
        line_send[i] = acc.astype(BF16)
        line_copy(i, here.z, z).start()

    groups = here.lines // per
    with jax.named_scope("groupA"):
        group(groups - 1)

    def later(k):
        g = groups - 1 - k
        group(g)
        loop(0, per, lambda j: pass_on((g + 1) * per + j))

    with jax.named_scope("later"):
        loop(1, groups, later)
    with jax.named_scope("passon"):
        loop(1, per, lambda j: pass_on(per - j))
    _, acc = quad_sum(0)
    total[...] += acc

    def add(i):
        z = (here.z + i) % here.lines
        line_copy(0, z, here.z).wait_recv()
        total[...] += line_buf[z].astype(F32)

    with jax.named_scope("addl"):
        loop(1, here.lines, add)
    joined[:, :wide] = (resid1[...] + rms_scale(total[...], g3[...])).astype(BF16)

    for copy in swaps:
        copy.wait_send()
    for plane in (first, third):
        plane.finish()
    for plane in (q_outs, tabs):
        plane.others(plane.wait_sent)

    def sent(z):
        for p in range(3):
            quad_copy(p, z).wait_send()

    loop(0, here.lines, sent)
    for p in range(2):
        quad_weight(p).wait_send()
        relay_weight(p).wait_send()
    for q in range(4):
        pair_weight(q).wait_send()
    for h in range(2):
        loop(1, here.lines, lambda i: line_rows(i, h).wait_send())
    loop(1, here.lines, lambda i: line_outs(i).wait_send())
    loop(1, here.lines, lambda i: line_copy(i, 0, here.z).wait_send())


def split_kernel(joined, layer_out, new_keys, new_values):
    wide, keys = layer_out.shape[1], new_keys.shape[1]
    layer_out[...] = joined[:, :wide]
    new_keys[...] = joined[:, wide:wide + keys]
    new_values[...] = joined[:, wide + keys:]


def run_layer(n, lens, tokens, gains, bias, routes, route_weights, wq, wk, wv, wo, ck, cv, eg, eu, ed, sg, su, sd):
    vm = pl.BlockSpec(memory_space=pltpu.VMEM)
    hbm = pl.BlockSpec(memory_space=pl.ANY)
    seqs, wide = tokens.shape
    own = wq.shape[0]
    ff = eg.shape[2]
    lines = n // 4
    pairs = n * 2 * own // LANES
    sems = pltpu.SemaphoreType.DMA
    half = lambda *shape: pltpu.VMEM(shape, BF16)
    full = lambda *shape: pltpu.VMEM(shape, F32)
    joined = pl.pallas_call(
        functools.partial(layer_kernel, n),
        out_shape=jax.ShapeDtypeStruct((seqs, wide + wk.shape[1] + wv.shape[1]), BF16),
        in_specs=[pl.BlockSpec(memory_space=pltpu.SMEM)] + [vm] * 8 + [hbm] * 12,
        out_specs=vm,
        scratch_shapes=[
            half(seqs, wide), half(n, seqs, wide), half(seqs, wide), half(lines, seqs, wide),
            half(seqs, wide), half(n, seqs, wide),
            half(2 * own, wide), half(wide, 2 * own), half(4, 2 * own, wide),
            half(*wk.shape), half(*wv.shape), half(*ck.shape), half(*cv.shape),
            half(LANES, 2 * LANES), full(seqs, pairs, LANES), full(seqs, pairs, LANES),
            half(n, seqs, 2 * own), half(n, seqs, 2 * own),
            half(lines, seqs, 8 * own), half(lines, seqs, 8 * own),
            full(seqs, wide), full(n, 2, LANES), full(n, 2, LANES), full(bias.shape[1], 1),
            half(2, wide, ff), half(2, wide, ff), half(2 * ff, wide),
            half(*sg.shape), half(*su.shape), half(*sd.shape),
            full(seqs, wide), half(n, seqs, wide), half(3, lines, seqs, wide),
            half(lines, seqs, wide), half(lines, seqs, wide),
            sems((3, n)), sems((n,)), sems((2, lines)), sems((2, lines)), sems((3, n)), sems((n,)),
            sems((n,)), sems((n,)), sems((lines,)), sems((lines,)), sems((n,)), sems((n,)),
            sems((4,)), sems((4,)), sems((3, lines)), sems((3, lines)),
            sems((lines,)), sems((lines,)), sems((2,)), sems((2,)), sems((2,)), sems((2,)),
            sems((4,)), sems((4,)), sems((12,)),
        ],
        compiler_params=pltpu.CompilerParams(
            collective_id=0, has_side_effects=True, vmem_limit_bytes=62 << 20
        ),
    )(lens, tokens, *gains, bias, routes, route_weights, wq, wk, wv, wo, ck, cv, eg, eu, ed, sg, su, sd)
    return pl.pallas_call(
        split_kernel,
        out_shape=(
            jax.ShapeDtypeStruct((seqs, wide), BF16),
            jax.ShapeDtypeStruct((seqs, wk.shape[1]), BF16),
            jax.ShapeDtypeStruct((seqs, wv.shape[1]), BF16),
        ),
        in_specs=[vm],
        out_specs=(vm,) * 3,
    )(joined)


def body(
    tokens,
    lengths,
    cache_keys,
    cache_values,
    mix_gain,
    mix_out_gain,
    ffn_gain,
    ffn_out_gain,
    query_weight,
    key_weight,
    value_weight,
    head_bias,
    output_weight,
    routes,
    route_weights,
    expert_gate,
    expert_up,
    expert_down,
    shared_gate,
    shared_up,
    shared_down,
):
    n = lax.axis_size("ep") // 2
    gains = [g[None] for g in (mix_gain, mix_out_gain, ffn_gain, ffn_out_gain)]
    return run_layer(
        n, lengths, tokens, gains, head_bias[None], routes.T, route_weights.T, query_weight.T, key_weight, value_weight,
        output_weight.T, cache_keys, cache_values,
        expert_gate, expert_up, expert_down, shared_gate, shared_up, shared_down,
    )


def solution(mesh):
    in_specs = (
        P("ep", None),
        P("ep"),
        P("ep", None, None),
        P("ep", None, None),
        P(),
        P(),
        P(),
        P(),
        P(None, "ep"),
        P(),
        P(),
        P(),
        P(None, "ep"),
        P("ep", None),
        P("ep", None),
        P("ep", None, None),
        P("ep", None, None),
        P("ep", None, None),
        P(),
        P(),
        P(),
    )
    out_specs = (P("ep", None), P("ep", None), P("ep", None))
    return jax.shard_map(body, mesh=mesh, in_specs=in_specs, out_specs=out_specs, check_vma=False)
```
